32 devices in a mesh: rep: 2 (over x), fs: 8 (over z, y), tp: 2 (over core).
Axes of the slice: x: 2, y: 2, z: 4, core: 2. Of those that a mesh axis runs over, the one named last changes fastest.
Arguments:
- tokens: bfloat16 [4096, 2048], P(('rep', 'fs')), may hold values from -6 to 6
- ffn_gate: bfloat16 [2048, 5632], P('fs', 'tp'), may hold values from -0.125 to 0.125
- ffn_up: bfloat16 [2048, 5632], P('fs', 'tp'), may hold values from -0.125 to 0.125
- ffn_down: bfloat16 [5632, 2048], P('tp', 'fs'), may hold values from -0.3125 to 0.3125
- query_proj: bfloat16 [2048, 512], P('fs', 'tp'), may hold values from -0.125 to 0.125
- key_proj: bfloat16 [2048, 512], P('fs', 'tp'), may hold values from -0.125 to 0.125
- value_proj: bfloat16 [2048, 1024], P('fs', 'tp'), may hold values from -0.125 to 0.125
- outgate_proj: bfloat16 [2048, 1024], P('fs', 'tp'), may hold values from -0.125 to 0.125
- output_proj: bfloat16 [1024, 2048], P('tp', 'fs'), may hold values from -0.375 to 0.375
- rank_down: bfloat16 [2048, 16], replicated, may hold values from -0.1875 to 0.1875
- rank_up: bfloat16 [16, 512], replicated, may hold values from -3 to 3
- decay_bias: float32 [512], replicated, may hold values from -0.5 to 8
- head_gain: float32 [1024], replicated, may hold values from 0.1 to 1.9
- norm_gain: float32 [3, 2048], replicated, may hold values from 0.1 to 1.9
- norm_bias: float32 [3, 2048], replicated, may hold values from -2 to 2
Outputs:
- layer_out: bfloat16 [4096, 2048], P(('rep', 'fs'))
The draws below stay inside these ranges and needn't reach their ends.
All inputs are finite; a program needn't handle non-finite values.
Results may differ from the reference program's by a relative error of at most 0.024.
Values may be sent and summed in bfloat16 or wider, within the bound.
No kernel may reach another device: no remote copies, remote signals or barrier semaphores. Data moves between devices by JAX's collectives and lax.ppermute only.
A program may use at most 128 MiB of HBM per device.

```python
import jax
import jax.numpy as jnp
from jax import lax

D = 2048
FF = 5632
HEADS = 8
DK = 64
DV = 128
RANK = 16
BLOCK = 64
TOK = 256
TOKENS = 4096
N_TP = 2


def draw_decay_bias(key, part):
    pick_key, slow_key, fast_key, jitter_key = jax.random.split(jax.random.fold_in(key, 11), 4)
    chance = 0.5
    slow_heads = jax.random.uniform(pick_key, (HEADS, 1), jnp.float32) < chance
    slow_level = jax.random.uniform(slow_key, (HEADS, 1), jnp.float32, 5.5, 7.5)
    fast_level = jax.random.uniform(fast_key, (HEADS, 1), jnp.float32, 0.0, 1.5)
    jitter = jax.random.uniform(jitter_key, (HEADS, DK), jnp.float32, -0.5, 0.5)
    return (jnp.where(slow_heads, slow_level, fast_level) + jitter).reshape(HEADS * DK).astype(jnp.float32)


def level_of(own_key, extent, shards, least, largest):
    factor_of, own = 1.0, jax.random.fold_in(own_key, 6)
    for axis_at, shards_of in shards:
        heights = jnp.exp(jax.random.uniform(jax.random.fold_in(own, axis_at), (shards_of,), jnp.float32, least / len(shards), largest / len(shards)))
        factor_of = factor_of * jnp.repeat(heights, extent[axis_at] // shards_of).reshape([-1 if axis == axis_at else 1 for axis in range(len(extent))])
    return factor_of


def bell_draw(key, extent, scale, bound, cuts=(), dtype=jnp.bfloat16):
    result = jax.random.normal(key, extent, jnp.float32) * scale
    if len(cuts) > 0:
        result = level_of(key, extent, cuts, -0.22, 0.18) * result
    return jnp.clip(result, min=-bound, max=bound).astype(dtype)


def setup_inputs(seed: int = 0) -> dict:
    splits = jax.random.split(jax.random.key(seed), 16)
    return {
        "tokens": bell_draw(splits[0], (TOKENS, D), 1.0, 6.0, ((0, 16),)),
        "ffn_gate": bell_draw(splits[1], (D, FF), D ** -0.5, 0.125, ((0, 8), (1, 2))),
        "ffn_up": bell_draw(splits[2], (D, FF), D ** -0.5, 0.125, ((0, 8), (1, 2))),
        "ffn_down": bell_draw(splits[3], (FF, D), (FF // 16) ** -0.5, 0.3125, ((0, 2), (1, 8))),
        "query_proj": bell_draw(splits[4], (D, HEADS * DK), D ** -0.5, 0.125, ((0, 8), (1, 2))),
        "key_proj": bell_draw(splits[5], (D, HEADS * DK), D ** -0.5, 0.125, ((0, 8), (1, 2))),
        "value_proj": bell_draw(splits[6], (D, HEADS * DV), D ** -0.5, 0.125, ((0, 8), (1, 2))),
        "outgate_proj": bell_draw(splits[7], (D, HEADS * DV), D ** -0.5, 0.125, ((0, 8), (1, 2))),
        "output_proj": bell_draw(splits[8], (HEADS * DV, D), (HEADS * DV // 4) ** -0.5, 0.375, ((0, 2), (1, 8))),
        "rank_down": bell_draw(splits[9], (D, RANK), (D // 2) ** -0.5, 0.1875),
        "rank_up": bell_draw(splits[10], (RANK, HEADS * DK), (RANK // 4) ** -0.5, 3.0),
        "decay_bias": draw_decay_bias(jax.random.fold_in(splits[15], 71), 0),
        "head_gain": jnp.clip(1.0 + 0.18 * jax.random.normal(splits[12], (HEADS * DV,), jnp.float32), 0.1, 1.9),
        "norm_gain": jnp.clip(1.0 + 0.18 * jax.random.normal(splits[13], (3, D), jnp.float32), 0.1, 1.9),
        "norm_bias": bell_draw(splits[14], (3, D), 0.3, 2.0, (), jnp.float32),
    }


EPSILON = 1e-05
HEAD_FLOOR = 1.0
RESIDUAL_SCALE = 2.0 ** 0.5
GATE_SOFTNESS = 16.0
FULL_ACCURACY = lax.Precision.HIGHEST

def layer_norm(summed, norm_gain, norm_shift):
    centred = summed - lax.optimization_barrier(jnp.mean(summed, -1, keepdims=True))
    spread = lax.optimization_barrier(jnp.mean(centred * centred, -1, keepdims=True))
    return (centred * lax.rsqrt(spread + EPSILON) * norm_gain + norm_shift).astype(jnp.bfloat16)

def gla_heads(queries, keys_rows, values, decay_logarithm):
    length, head_count, key_width = queries.shape
    value_width = values.shape[-1]
    block_count = length // BLOCK

    def blocks(array):
        return array.reshape(block_count, BLOCK, head_count, array.shape[-1])
    causal = jnp.tril(jnp.ones((BLOCK, BLOCK), bool))[:, :, None, None]

    def advance(running_state, inputs):
        query_block, key_block, value_block, decay_blk = inputs
        decay_prefix = jnp.cumsum(decay_blk, axis=0)
        spread = decay_prefix[:, None] - decay_prefix[None, :]
        weight = jnp.exp(jnp.where(causal, spread, -jnp.inf))
        scores = jnp.einsum('lshk,lhk,shk->hls', weight, query_block, key_block, precision=FULL_ACCURACY)
        within = jnp.einsum('hls,shv->lhv', scores, value_block, precision=FULL_ACCURACY)
        carried_over = jnp.einsum('zew,ewa->zea', query_block * jnp.exp(decay_prefix), running_state, precision=FULL_ACCURACY)
        block_finish = decay_prefix[-1]
        running_state = jnp.exp(block_finish)[:, :, None] * running_state + jnp.einsum('oct,ocy->cty', key_block * jnp.exp(block_finish[None] - decay_prefix), value_block, precision=FULL_ACCURACY)
        return (running_state, within + carried_over)
    initial = jnp.zeros((head_count, key_width, value_width), jnp.float32)
    _, outputs = lax.scan(advance, initial, (blocks(queries), blocks(keys_rows), blocks(values), blocks(decay_logarithm)))
    return outputs.reshape(length, head_count, value_width)

def block_partials(hidden, weight):
    width = weight.shape[0] // N_TP
    summed = jnp.zeros((hidden.shape[0], weight.shape[1]), jnp.float32)
    for block in range(N_TP):
        product = jnp.dot(hidden[:, block * width:(block + 1) * width], weight[block * width:(block + 1) * width], preferred_element_type=jnp.float32)
        rounded = lax.optimization_barrier(product.astype(jnp.bfloat16))
        summed = summed + rounded.astype(jnp.float32)
    return summed

def reference(tokens, ffn_gate, ffn_up, ffn_down, query_proj, key_proj, value_proj, outgate_proj, output_proj, rank_down, rank_up, decay_bias, head_gain, norm_gain, norm_bias):

    def channel_mix(normed):
        gate_rows = jnp.dot(normed, ffn_gate, preferred_element_type=jnp.float32)
        up_rows = jnp.dot(normed, ffn_up, preferred_element_type=jnp.float32)
        hidden = (jax.nn.silu(gate_rows) * up_rows).astype(jnp.bfloat16)
        return block_partials(hidden, ffn_down)

    def one_sequence(rows):
        first = layer_norm(RESIDUAL_SCALE * rows.astype(jnp.float32) + 0.5 * channel_mix(rows), norm_gain[0], norm_bias[0])
        queries = jnp.dot(first, query_proj, preferred_element_type=jnp.float32) * DK ** (-0.5)
        keys_rows = jnp.dot(first, key_proj, preferred_element_type=jnp.float32)
        values = jnp.dot(first, value_proj, preferred_element_type=jnp.float32)
        gates = jnp.dot(first, outgate_proj, preferred_element_type=jnp.float32)
        rank_rows = jnp.dot(first, rank_down, preferred_element_type=jnp.float32)
        decay_source = jnp.dot(rank_rows, rank_up.astype(jnp.float32), precision=FULL_ACCURACY) + decay_bias
        decay_logarithm = jax.nn.log_sigmoid(decay_source) / GATE_SOFTNESS
        length = rows.shape[0]
        heads_out = gla_heads(queries.reshape(length, HEADS, DK), keys_rows.reshape(length, HEADS, DK), values.reshape(length, HEADS, DV), decay_logarithm.reshape(length, HEADS, DK))
        scaled = heads_out * lax.rsqrt(lax.optimization_barrier(jnp.mean(heads_out * heads_out, -1, keepdims=True)) + HEAD_FLOOR)
        scaled = scaled * head_gain.reshape(HEADS, DV)
        mixed = (scaled.reshape(length, HEADS * DV) * jax.nn.silu(gates)).astype(jnp.bfloat16)
        second = layer_norm(RESIDUAL_SCALE * first.astype(jnp.float32) + block_partials(mixed, output_proj), norm_gain[1], norm_bias[1])
        return layer_norm(RESIDUAL_SCALE * second.astype(jnp.float32) + 0.5 * channel_mix(second), norm_gain[2], norm_bias[2])
    sequences = tokens.reshape(TOKENS // TOK, TOK, D)
    return lax.map(one_sequence, sequences).reshape(TOKENS, D)
```

```python
import functools

import jax
import jax.numpy as jnp
from jax import lax
from jax.experimental import pallas as pl
from jax.experimental.pallas import tpu as pltpu
from jax.sharding import PartitionSpec as P

DK = 64
DV = 128

EPSILON = 1e-05
HEAD_FLOOR = 1.0
RESIDUAL_SCALE = 2.0**0.5
GATE_SOFTNESS = 16.0
FULL_ACCURACY = lax.Precision.HIGHEST
MAX_SHARD_REFS = 8
TILE = 256


def dot32(a, b):
    return jnp.dot(a, b, preferred_element_type=jnp.float32)


class Ring:
    def __init__(self, sizes):
        self.n = sizes["fs"]
        self.ny = 2 if self.n % 2 == 0 else 1
        self.nz = self.n // self.ny
        self.nr = sizes["rep"]
        self.index = lax.axis_index("fs")
        self.rep = lax.axis_index("rep") if self.nr == 2 else 0
        ny, nz = self.ny, self.nz
        self.z_pairs = [(z * ny + y, (z + 1) % nz * ny + y) for z in range(nz) for y in range(ny)]
        self.y_pairs = [(z * ny + y, z * ny + (y + 1) % ny) for z in range(nz) for y in range(ny)]

    def source(self, j):
        z, y = self.index // self.ny, self.index % self.ny
        dz, dy = j // self.ny, j % self.ny
        return (z - dz) % self.nz * self.ny + (y - dy) % self.ny

    def place(self, shard):
        z, y = self.index // self.ny, self.index % self.ny
        za, ya = shard // self.ny, shard % self.ny
        return (z - za) % self.nz * self.ny + (y - ya) % self.ny

    def gather(self, own):
        pieces = []
        at_z = own
        for dz in range(self.nz):
            if dz:
                at_z = lax.ppermute(at_z, "fs", self.z_pairs)
            pieces.append(at_z)
            at_y = at_z
            for _ in range(self.ny - 1):
                at_y = lax.ppermute(at_y, "fs", self.y_pairs)
                pieces.append(at_y)
        return pieces

    def gather_split(self, weight, axis, outer):
        inner = weight.shape[axis] - 2 * outer
        step = outer + inner
        shared = self.gather(lax.slice_in_dim(weight, outer, step, axis=axis))
        if self.nr != 2:
            first = self.gather(lax.slice_in_dim(weight, 0, outer, axis=axis))
            last = self.gather(lax.slice_in_dim(weight, step, step + outer, axis=axis))
            return first, shared, last
        own = self.gather(lax.dynamic_slice_in_dim(weight, self.rep * step, outer, axis))
        other = [lax.dynamic_slice_in_dim(weight, (1 - self.rep) * step, outer, axis)]
        other += [lax.ppermute(piece, "rep", [(0, 1), (1, 0)]) for piece in own[1:]]
        return own, shared, other

    def reorder(self, array, axis):
        width = array.shape[axis] // self.n
        return jnp.concatenate(
            [
                lax.dynamic_slice_in_dim(array, self.source(j) * width, width, axis)
                for j in range(self.n)
            ],
            axis,
        )

    def restore(self, array, axis):
        width = array.shape[axis] // self.n
        return jnp.concatenate(
            [
                lax.dynamic_slice_in_dim(array, self.place(s) * width, width, axis)
                for s in range(self.n)
            ],
            axis,
        )


def bundle(shards, axis):
    group = -(-len(shards) // MAX_SHARD_REFS)
    if group == 1:
        return shards
    return [
        jnp.concatenate(shards[i : i + group], axis) for i in range(0, len(shards), group)
    ]


def tile_of(width):
    return TILE if width % TILE == 0 else width


def held(start, count):
    return lambda i: jnp.clip(i - start, 0, count - 1)


def rows_product(rows, shard_refs):
    total = None
    at = 0
    for ref in shard_refs:
        depth = ref.shape[0]
        part = dot32(rows[:, at : at + depth], ref[...])
        total = part if total is None else total + part
        at += depth
    return total


def spans_of(widths):
    spans, start = [], 0
    for width in widths:
        count = width // tile_of(width)
        spans.append((start, count))
        start += count
    return spans, start


def gated_hidden(rows, gate_parts, up_parts):
    widths = [part[0].shape[1] for part in gate_parts]
    spans, steps = spans_of(widths)
    m = len(gate_parts[0])
    parts = len(widths)

    def body(*refs):
        rows_ref = refs[0]
        weights = refs[1 : 1 + 2 * parts * m]
        outs = refs[1 + 2 * parts * m :]
        i = pl.program_id(0)
        for p, (start, count) in enumerate(spans):

            @pl.when((i >= start) & (i < start + count))
            def _(p=p):
                rows_now = rows_ref[...]
                gate = rows_product(rows_now, weights[2 * p * m : (2 * p + 1) * m])
                up = rows_product(rows_now, weights[(2 * p + 1) * m : (2 * p + 2) * m])
                outs[p][...] = (gate / (1.0 + jnp.exp(-gate)) * up).astype(jnp.bfloat16)

    def spec(height, width, span):
        at = held(*span)
        return pl.BlockSpec((height, tile_of(width)), lambda i: (0, at(i)))

    in_specs = [pl.BlockSpec(rows.shape, lambda i: (0, 0))]
    operands = [rows]
    for p in range(parts):
        for shard in list(gate_parts[p]) + list(up_parts[p]):
            in_specs.append(spec(shard.shape[0], widths[p], spans[p]))
            operands.append(shard)
    count = rows.shape[0]
    return pl.pallas_call(
        body,
        grid=(steps,),
        in_specs=in_specs,
        out_specs=[spec(count, widths[p], spans[p]) for p in range(parts)],
        out_shape=[jax.ShapeDtypeStruct((count, w), jnp.bfloat16) for w in widths],
        name="gated_hidden",
    )(*operands)


def columns_product(hidden_parts, down_parts):
    widths = [hidden.shape[1] for hidden in hidden_parts]
    spans, steps = spans_of(widths)
    m = len(down_parts[0])
    parts = len(widths)
    count = hidden_parts[0].shape[0]
    columns = [shard.shape[1] for shard in down_parts[0]]
    total = sum(columns)

    def body(*refs):
        hidden_refs = refs[:parts]
        weights = refs[parts : parts + parts * m]
        out_ref, sum_ref = refs[-2:]
        i = pl.program_id(0)

        @pl.when(i == 0)
        def _():
            sum_ref[...] = jnp.zeros(sum_ref.shape, jnp.float32)

        for p, (start, steps_here) in enumerate(spans):

            @pl.when((i >= start) & (i < start + steps_here))
            def _(p=p):
                hidden_now = hidden_refs[p][...]
                at = 0
                for k in range(m):
                    width = columns[k]
                    sum_ref[:, at : at + width] += dot32(hidden_now, weights[p * m + k][...])
                    at += width

        @pl.when(i == steps - 1)
        def _():
            out_ref[...] = sum_ref[...].astype(jnp.bfloat16)

    def hidden_spec(width, span):
        at = held(*span)
        return pl.BlockSpec((count, tile_of(width)), lambda i: (0, at(i)))

    def down_spec(width, cols, span):
        at = held(*span)
        return pl.BlockSpec((tile_of(width), cols), lambda i: (at(i), 0))

    in_specs = [hidden_spec(widths[p], spans[p]) for p in range(parts)]
    operands = list(hidden_parts)
    for p in range(parts):
        for shard in down_parts[p]:
            in_specs.append(down_spec(widths[p], shard.shape[1], spans[p]))
            operands.append(shard)
    return pl.pallas_call(
        body,
        grid=(steps,),
        in_specs=in_specs,
        out_specs=pl.BlockSpec((count, total), lambda i: (0, 0)),
        out_shape=jax.ShapeDtypeStruct((count, total), jnp.bfloat16),
        scratch_shapes=[pltpu.VMEM((count, total), jnp.float32)],
        name="columns_product",
    )(*operands)


def projection(rows, parts):
    m = len(parts[0])

    def body(*refs):
        rows_now = refs[0][...]
        for p in range(len(parts)):
            product = rows_product(rows_now, refs[1 + p * m : 1 + (p + 1) * m])
            refs[1 + len(parts) * m + p][...] = product

    return pl.pallas_call(
        body,
        out_shape=[
            jax.ShapeDtypeStruct((rows.shape[0], part[0].shape[1]), jnp.float32) for part in parts
        ],
        name="projection",
    )(rows, *[shard for part in parts for shard in part])


def mixer_body(
    first_ref, down_ref, up_ref, bias_ref, qk_ref, values_ref, gates_ref, gain_ref, out_ref
):
    length, value_cols = values_ref.shape
    key_cols = qk_ref.shape[1] // 2
    head_count = key_cols // DK
    source = (
        jnp.dot(
            dot32(first_ref[...], down_ref[...]),
            up_ref[...].astype(jnp.float32),
            precision=FULL_ACCURACY,
            preferred_element_type=jnp.float32,
        )
        + bias_ref[...]
    )
    logarithm = jnp.minimum(source, 0.0) - jnp.log1p(jnp.exp(-jnp.abs(source)))
    decay = logarithm * (1.0 / GATE_SOFTNESS)
    decay_high = decay.astype(jnp.bfloat16)
    rest = decay - decay_high.astype(jnp.float32)
    decay_mid = rest.astype(jnp.bfloat16)
    decay_low = (rest - decay_mid.astype(jnp.float32)).astype(jnp.bfloat16)
    queries = qk_ref[:, :key_cols] * DK ** (-0.5)
    keys = qk_ref[:, key_cols:]

    row = lax.broadcasted_iota(jnp.int32, (length, length), 0)
    col = lax.broadcasted_iota(jnp.int32, (length, length), 1)
    position = lax.broadcasted_iota(jnp.int32, (length, key_cols), 0)
    channel = lax.broadcasted_iota(jnp.int32, (length, key_cols), 1)
    contract = (((1,), (1,)), ((), ()))

    def head_scores(query_side, key_side):
        query_side = query_side.astype(jnp.bfloat16)
        result = []
        for head in range(head_count):
            if head_count > 1:
                key_now = jnp.where(channel // DK == head, key_side, 0.0)
            else:
                key_now = key_side
            result.append(
                lax.dot_general(
                    query_side,
                    key_now.astype(jnp.bfloat16),
                    contract,
                    preferred_element_type=jnp.float32,
                )
            )
        return result

    scores = [jnp.where(row == col, s, 0.0) for s in head_scores(queries, keys)]
    half = 1
    while half < length:
        border = row // (2 * half) * (2 * half) + half
        above = (row >= border) & (col >= border) & (col <= row)
        below = (row < border) & (col > row) & (col < border)
        select = jnp.where(above | below, 1.0, 0.0).astype(jnp.bfloat16)
        exponent = dot32(select, decay_high) + dot32(select, decay_mid) + dot32(select, decay_low)
        factor = jnp.exp(exponent)
        upper = position // half % 2 == 1
        query_side = jnp.where(upper, queries * factor, 0.0)
        key_side = jnp.where(upper, 0.0, keys * factor)
        together = row // (2 * half) == col // (2 * half)
        for head, s in enumerate(head_scores(query_side, key_side)):
            scores[head] += s if 2 * half >= length else jnp.where(together, s, 0.0)
        half *= 2
    for head in range(head_count):
        channels = slice(head * DV, (head + 1) * DV)
        heads_out = dot32(
            scores[head].astype(jnp.bfloat16), values_ref[:, channels].astype(jnp.bfloat16)
        )
        scaled = heads_out * lax.rsqrt(
            jnp.mean(heads_out * heads_out, -1, keepdims=True) + HEAD_FLOOR
        )
        gates = gates_ref[:, channels]
        out_ref[:, channels] = (
            scaled * gain_ref[:, channels] * (gates / (1.0 + jnp.exp(-gates)))
        ).astype(jnp.bfloat16)


def layer_norm(summed, norm_gain, norm_shift):
    centred = summed - jnp.mean(summed, -1, keepdims=True)
    spread = jnp.mean(centred * centred, -1, keepdims=True)
    return (centred * lax.rsqrt(spread + EPSILON) * norm_gain + norm_shift).astype(jnp.bfloat16)


def settle(partial_value, tp_size, residual_rows, factor, norm_gain, norm_shift):
    if tp_size == 2:
        other = lax.ppermute(partial_value, "tp", [(0, 1), (1, 0)])
        summed = partial_value.astype(jnp.float32) + other.astype(jnp.float32)
    else:
        summed = lax.psum(partial_value, "tp").astype(jnp.float32)
    return layer_norm(
        RESIDUAL_SCALE * residual_rows.astype(jnp.float32) + factor * summed, norm_gain, norm_shift
    )


def per_device(
    sizes,
    tokens,
    ffn_gate,
    ffn_up,
    ffn_down,
    query_proj,
    key_proj,
    value_proj,
    outgate_proj,
    output_proj,
    rank_down,
    rank_up,
    decay_bias,
    head_gain,
    norm_gain,
    norm_bias,
):
    ring = Ring(sizes)
    tp_size = sizes["tp"]
    hidden_cols = ffn_gate.shape[1]
    unit = 64 if hidden_cols % 64 == 0 else 1
    outer = hidden_cols * 4 // 11 // unit * unit
    gate_parts = [bundle(p, 0) for p in ring.gather_split(ffn_gate, 1, outer)]
    up_parts = [bundle(p, 0) for p in ring.gather_split(ffn_up, 1, outer)]
    down_parts = [bundle(p, 1) for p in ring.gather_split(ffn_down, 0, outer)]
    value_cols = value_proj.shape[1]
    key_cols = query_proj.shape[1]
    joined = jnp.concatenate([query_proj, key_proj, value_proj, outgate_proj], axis=1)
    joined_parts = [bundle(p, 0) for p in ring.gather_split(joined, 1, value_cols)]
    output_shards = bundle(ring.gather(output_proj), 1)

    rows = ring.reorder(tokens, 1)
    gains = ring.reorder(norm_gain, 1)
    shifts = ring.reorder(norm_bias, 1)
    rank_rows = ring.reorder(rank_down, 0)

    def channel_mix(normed):
        return columns_product(gated_hidden(normed, gate_parts, up_parts), down_parts)

    first = settle(channel_mix(rows), tp_size, rows, 0.5, gains[0], shifts[0])
    mine, shared, others = projection(first, joined_parts)
    qk = jnp.where(ring.rep == 0, mine, others)
    gates = jnp.where(ring.rep == 0, others, mine)
    position = lax.axis_index("tp")
    up_block = lax.dynamic_slice_in_dim(rank_up, position * key_cols, key_cols, 1)
    bias_block = lax.dynamic_slice_in_dim(decay_bias, position * key_cols, key_cols, 0)
    gain_block = lax.dynamic_slice_in_dim(head_gain, position * value_cols, value_cols, 0)
    mixed = pl.pallas_call(
        mixer_body,
        out_shape=jax.ShapeDtypeStruct((first.shape[0], value_cols), jnp.bfloat16),
        name="mixer",
    )(first, rank_rows, up_block, bias_block[None], qk, shared, gates, gain_block[None])
    second = settle(
        columns_product([mixed], [output_shards]), tp_size, first, 1.0, gains[1], shifts[1]
    )
    last = settle(channel_mix(second), tp_size, second, 0.5, gains[2], shifts[2])
    return ring.restore(last, 1)


def solution(mesh):
    return jax.shard_map(
        functools.partial(per_device, dict(mesh.shape)),
        mesh=mesh,
        in_specs=(
            P(("rep", "fs"), None),
            P("fs", "tp"),
            P("fs", "tp"),
            P("tp", "fs"),
            P("fs", "tp"),
            P("fs", "tp"),
            P("fs", "tp"),
            P("fs", "tp"),
            P("tp", "fs"),
            P(),
            P(),
            P(),
            P(),
            P(),
            P(),
        ),
        out_specs=P(("rep", "fs"), None),
        check_vma=False,
    )
```

```python
import functools

import jax
import jax.numpy as jnp
from jax import lax
from jax.experimental import pallas as pl
from jax.experimental.pallas import tpu as pltpu
from jax.sharding import PartitionSpec as P

DK = 64
DV = 128

EPSILON = 1e-05
HEAD_FLOOR = 1.0
RESIDUAL_SCALE = 2.0**0.5
GATE_SOFTNESS = 16.0
FULL_ACCURACY = lax.Precision.HIGHEST
MAX_SHARD_REFS = 8
TILE = 256


def dot32(a, b):
    return jnp.dot(a, b, preferred_element_type=jnp.float32)


class Ring:
    def __init__(self, sizes):
        self.n = sizes["fs"]
        self.ny = 2 if self.n % 2 == 0 else 1
        self.nz = self.n // self.ny
        self.nr = sizes["rep"]
        self.index = lax.axis_index("fs")
        self.rep = lax.axis_index("rep") if self.nr == 2 else 0
        ny, nz = self.ny, self.nz
        self.z_pairs = [(z * ny + y, (z + 1) % nz * ny + y) for z in range(nz) for y in range(ny)]
        self.y_pairs = [(z * ny + y, z * ny + (y + 1) % ny) for z in range(nz) for y in range(ny)]

    def source(self, j):
        z, y = self.index // self.ny, self.index % self.ny
        dz, dy = j // self.ny, j % self.ny
        return (z - dz) % self.nz * self.ny + (y - dy) % self.ny

    def place(self, shard):
        z, y = self.index // self.ny, self.index % self.ny
        za, ya = shard // self.ny, shard % self.ny
        return (z - za) % self.nz * self.ny + (y - ya) % self.ny

    def parts(self, weight, axis, outer):
        if self.nr != 2:
            return weight, None
        width = weight.shape[axis] - outer
        part = lax.dynamic_slice_in_dim(weight, self.rep * outer, width, axis)
        return part, lax.dynamic_slice_in_dim(weight, (1 - self.rep) * width, outer, axis)

    def gather(self, early, late):
        n, ny, nz = self.n, self.ny, self.nz
        rounds, crossing, waiting = [], [], []

        def run(moves, fenced=True):
            if not moves:
                return
            values = [move[0] for move in moves]
            if fenced and len(rounds) >= 2:
                values, _ = lax.optimization_barrier((values, rounds[-2]))
            arrived = []
            for value, (_, name, pairs, keep) in zip(values, moves):
                arrived.append(lax.ppermute(value, name, pairs))
                keep(arrived[-1])
            if fenced:
                rounds.append(arrived)

        def take(limit):
            now = crossing[:limit]
            del crossing[:limit]
            return [(cut(), "rep", [(0, 1), (1, 0)], keep) for cut, keep in now]

        def entry_of(weight, axis, outer):
            main, rest = (weight, None) if outer is None else self.parts(weight, axis, outer)
            shards = [main] + [None] * (n - 1)
            return shards, None if rest is None else [rest] + [None] * (n - 1), axis, outer

        def land(entry, j):
            shards, others, axis, outer = entry

            def keep(value):
                shards[j] = value
                if others is None:
                    return

                def cut():
                    inner = value.shape[axis] - outer
                    return lax.dynamic_slice_in_dim(value, self.rep * inner, outer, axis)

                queue = crossing if any(entry is e for e in soon) else waiting
                queue.append((cut, functools.partial(others.__setitem__, j)))

            return keep

        def along_y(entry, dz):
            if ny != 2:
                return []
            return [(entry[0][dz * ny], "fs", self.y_pairs, land(entry, dz * ny + 1))]

        def along_z(entry, dz):
            if dz + 1 >= nz:
                return []
            return [(entry[0][dz * ny], "fs", self.z_pairs, land(entry, (dz + 1) * ny))]

        soon = [entry_of(*item) for item in early]
        then = [entry_of(*item) for item in late]
        hop = 0
        for dz in range(nz):
            for entry in soon:
                moves = take(2) + along_y(entry, dz)
                if dz + 1 < nz:
                    moves += along_z(entry, dz)
                    run(moves)
                    continue
                for other in then:
                    moves += along_z(other, hop)
                hop += 1
                run(moves)
        while hop + 1 < nz:
            run([move for other in then for move in along_z(other, hop)])
            hop += 1
        crossing += waiting
        waiting.clear()
        run(take(len(crossing)) + [m for other in then for dz in range(nz) for m in along_y(other, dz)])
        crossing += waiting
        run(take(len(crossing)), fenced=False)
        return [[e[0]] if e[1] is None else [e[0], e[1]] for e in soon + then]

    def reorder(self, array, axis):
        width = array.shape[axis] // self.n
        return jnp.concatenate(
            [
                lax.dynamic_slice_in_dim(array, self.source(j) * width, width, axis)
                for j in range(self.n)
            ],
            axis,
        )

    def restore(self, array, axis):
        width = array.shape[axis] // self.n
        return jnp.concatenate(
            [
                lax.dynamic_slice_in_dim(array, self.place(s) * width, width, axis)
                for s in range(self.n)
            ],
            axis,
        )


def bundle(shards, axis):
    group = -(-len(shards) // MAX_SHARD_REFS)
    if group == 1:
        return shards
    return [
        jnp.concatenate(shards[i : i + group], axis) for i in range(0, len(shards), group)
    ]


def tile_of(width):
    return TILE if width % TILE == 0 else width


def held(start, count):
    return lambda i: jnp.clip(i - start, 0, count - 1)


def rows_product(rows, shard_refs):
    total = None
    at = 0
    for ref in shard_refs:
        depth = ref.shape[0]
        part = dot32(rows[:, at : at + depth], ref[...])
        total = part if total is None else total + part
        at += depth
    return total


def spans_of(widths):
    spans, start = [], 0
    for width in widths:
        count = width // tile_of(width)
        spans.append((start, count))
        start += count
    return spans, start


def gated_hidden(rows, gate_parts, up_parts):
    widths = [part[0].shape[1] for part in gate_parts]
    spans, steps = spans_of(widths)
    m = len(gate_parts[0])
    parts = len(widths)

    def body(*refs):
        rows_ref = refs[0]
        weights = refs[1 : 1 + 2 * parts * m]
        outs = refs[1 + 2 * parts * m :]
        i = pl.program_id(0)
        for p, (start, count) in enumerate(spans):

            @pl.when((i >= start) & (i < start + count))
            def _(p=p):
                rows_now = rows_ref[...]
                gate = rows_product(rows_now, weights[2 * p * m : (2 * p + 1) * m])
                up = rows_product(rows_now, weights[(2 * p + 1) * m : (2 * p + 2) * m])
                outs[p][...] = (gate / (1.0 + jnp.exp(-gate)) * up).astype(jnp.bfloat16)

    def spec(height, width, span):
        at = held(*span)
        return pl.BlockSpec((height, tile_of(width)), lambda i: (0, at(i)))

    in_specs = [pl.BlockSpec(rows.shape, lambda i: (0, 0))]
    operands = [rows]
    for p in range(parts):
        for shard in list(gate_parts[p]) + list(up_parts[p]):
            in_specs.append(spec(shard.shape[0], widths[p], spans[p]))
            operands.append(shard)
    count = rows.shape[0]
    return pl.pallas_call(
        body,
        grid=(steps,),
        in_specs=in_specs,
        out_specs=[spec(count, widths[p], spans[p]) for p in range(parts)],
        out_shape=[jax.ShapeDtypeStruct((count, w), jnp.bfloat16) for w in widths],
        name="gated_hidden",
    )(*operands)


def columns_product(hidden_parts, down_parts):
    widths = [hidden.shape[1] for hidden in hidden_parts]
    spans, steps = spans_of(widths)
    m = len(down_parts[0])
    parts = len(widths)
    count = hidden_parts[0].shape[0]
    columns = [shard.shape[1] for shard in down_parts[0]]
    total = sum(columns)

    def body(*refs):
        hidden_refs = refs[:parts]
        weights = refs[parts : parts + parts * m]
        out_ref, sum_ref = refs[-2:]
        i = pl.program_id(0)

        @pl.when(i == 0)
        def _():
            sum_ref[...] = jnp.zeros(sum_ref.shape, jnp.float32)

        for p, (start, steps_here) in enumerate(spans):

            @pl.when((i >= start) & (i < start + steps_here))
            def _(p=p):
                hidden_now = hidden_refs[p][...]
                at = 0
                for k in range(m):
                    width = columns[k]
                    sum_ref[:, at : at + width] += dot32(hidden_now, weights[p * m + k][...])
                    at += width

        @pl.when(i == steps - 1)
        def _():
            out_ref[...] = sum_ref[...].astype(jnp.bfloat16)

    def hidden_spec(width, span):
        at = held(*span)
        return pl.BlockSpec((count, tile_of(width)), lambda i: (0, at(i)))

    def down_spec(width, cols, span):
        at = held(*span)
        return pl.BlockSpec((tile_of(width), cols), lambda i: (at(i), 0))

    in_specs = [hidden_spec(widths[p], spans[p]) for p in range(parts)]
    operands = list(hidden_parts)
    for p in range(parts):
        for shard in down_parts[p]:
            in_specs.append(down_spec(widths[p], shard.shape[1], spans[p]))
            operands.append(shard)
    return pl.pallas_call(
        body,
        grid=(steps,),
        in_specs=in_specs,
        out_specs=pl.BlockSpec((count, total), lambda i: (0, 0)),
        out_shape=jax.ShapeDtypeStruct((count, total), jnp.bfloat16),
        scratch_shapes=[pltpu.VMEM((count, total), jnp.float32)],
        name="columns_product",
    )(*operands)


def projection(rows, parts):
    m = len(parts[0])

    def body(*refs):
        rows_now = refs[0][...]
        for p in range(len(parts)):
            product = rows_product(rows_now, refs[1 + p * m : 1 + (p + 1) * m])
            refs[1 + len(parts) * m + p][...] = product

    return pl.pallas_call(
        body,
        out_shape=[
            jax.ShapeDtypeStruct((rows.shape[0], part[0].shape[1]), jnp.float32) for part in parts
        ],
        name="projection",
    )(rows, *[shard for part in parts for shard in part])


def mixer_body(
    first_ref, down_ref, up_ref, bias_ref, qk_ref, values_ref, gates_ref, gain_ref, out_ref
):
    length, value_cols = values_ref.shape
    key_cols = qk_ref.shape[1] // 2
    head_count = key_cols // DK
    source = (
        jnp.dot(
            dot32(first_ref[...], down_ref[...]),
            up_ref[...].astype(jnp.float32),
            precision=FULL_ACCURACY,
            preferred_element_type=jnp.float32,
        )
        + bias_ref[...]
    )
    logarithm = jnp.minimum(source, 0.0) - jnp.log1p(jnp.exp(-jnp.abs(source)))
    decay = logarithm * (1.0 / GATE_SOFTNESS)
    decay_high = decay.astype(jnp.bfloat16)
    rest = decay - decay_high.astype(jnp.float32)
    decay_mid = rest.astype(jnp.bfloat16)
    decay_low = (rest - decay_mid.astype(jnp.float32)).astype(jnp.bfloat16)
    queries = qk_ref[:, :key_cols] * DK ** (-0.5)
    keys = qk_ref[:, key_cols:]

    row = lax.broadcasted_iota(jnp.int32, (length, length), 0)
    col = lax.broadcasted_iota(jnp.int32, (length, length), 1)
    position = lax.broadcasted_iota(jnp.int32, (length, key_cols), 0)
    channel = lax.broadcasted_iota(jnp.int32, (length, key_cols), 1)
    contract = (((1,), (1,)), ((), ()))

    def head_scores(query_side, key_side):
        query_side = query_side.astype(jnp.bfloat16)
        result = []
        for head in range(head_count):
            if head_count > 1:
                key_now = jnp.where(channel // DK == head, key_side, 0.0)
            else:
                key_now = key_side
            result.append(
                lax.dot_general(
                    query_side,
                    key_now.astype(jnp.bfloat16),
                    contract,
                    preferred_element_type=jnp.float32,
                )
            )
        return result

    scores = [jnp.where(row == col, s, 0.0) for s in head_scores(queries, keys)]
    half = 1
    while half < length:
        border = row // (2 * half) * (2 * half) + half
        above = (row >= border) & (col >= border) & (col <= row)
        below = (row < border) & (col > row) & (col < border)
        select = jnp.where(above | below, 1.0, 0.0).astype(jnp.bfloat16)
        exponent = dot32(select, decay_high) + dot32(select, decay_mid) + dot32(select, decay_low)
        factor = jnp.exp(exponent)
        upper = position // half % 2 == 1
        query_side = jnp.where(upper, queries * factor, 0.0)
        key_side = jnp.where(upper, 0.0, keys * factor)
        together = row // (2 * half) == col // (2 * half)
        for head, s in enumerate(head_scores(query_side, key_side)):
            scores[head] += s if 2 * half >= length else jnp.where(together, s, 0.0)
        half *= 2
    for head in range(head_count):
        channels = slice(head * DV, (head + 1) * DV)
        heads_out = dot32(
            scores[head].astype(jnp.bfloat16), values_ref[:, channels].astype(jnp.bfloat16)
        )
        scaled = heads_out * lax.rsqrt(
            jnp.mean(heads_out * heads_out, -1, keepdims=True) + HEAD_FLOOR
        )
        gates = gates_ref[:, channels]
        out_ref[:, channels] = (
            scaled * gain_ref[:, channels] * (gates / (1.0 + jnp.exp(-gates)))
        ).astype(jnp.bfloat16)


def layer_norm(summed, norm_gain, norm_shift):
    centred = summed - jnp.mean(summed, -1, keepdims=True)
    spread = jnp.mean(centred * centred, -1, keepdims=True)
    return (centred * lax.rsqrt(spread + EPSILON) * norm_gain + norm_shift).astype(jnp.bfloat16)


def settle(partial_value, tp_size, residual_rows, factor, norm_gain, norm_shift):
    if tp_size == 2:
        other = lax.ppermute(partial_value, "tp", [(0, 1), (1, 0)])
        summed = partial_value.astype(jnp.float32) + other.astype(jnp.float32)
    else:
        summed = lax.psum(partial_value, "tp").astype(jnp.float32)
    return layer_norm(
        RESIDUAL_SCALE * residual_rows.astype(jnp.float32) + factor * summed, norm_gain, norm_shift
    )


def per_device(
    sizes,
    tokens,
    ffn_gate,
    ffn_up,
    ffn_down,
    query_proj,
    key_proj,
    value_proj,
    outgate_proj,
    output_proj,
    rank_down,
    rank_up,
    decay_bias,
    head_gain,
    norm_gain,
    norm_bias,
):
    ring = Ring(sizes)
    tp_size = sizes["tp"]
    hidden_cols = ffn_gate.shape[1]
    unit = 64 if hidden_cols % 64 == 0 else 1
    outer = hidden_cols * 4 // 11 // unit * unit
    value_cols = value_proj.shape[1]
    key_cols = query_proj.shape[1]
    joined = jnp.concatenate([query_proj, key_proj, value_proj, outgate_proj], axis=1)
    gathered = ring.gather(
        [(ffn_gate, 1, outer), (ffn_up, 1, outer), (ffn_down, 0, outer)],
        [(joined, 1, value_cols), (output_proj, 1, None)],
    )
    axes = (0, 0, 1, 0, 1)
    gate_parts, up_parts, down_parts, joined_parts, (output_shards,) = [
        [bundle(part, axis) for part in parts] for parts, axis in zip(gathered, axes)
    ]

    rows = ring.reorder(tokens, 1)
    gains = ring.reorder(norm_gain, 1)
    shifts = ring.reorder(norm_bias, 1)
    rank_rows = ring.reorder(rank_down, 0)

    def channel_mix(normed):
        return columns_product(gated_hidden(normed, gate_parts, up_parts), down_parts)

    first = settle(channel_mix(rows), tp_size, rows, 0.5, gains[0], shifts[0])
    projected = projection(first, joined_parts)
    if len(projected) == 1:
        qk, values, gates = jnp.split(projected[0], 3, 1)
    else:
        left, right = jnp.split(projected[0], 2, 1)
        low = ring.rep == 0
        qk = jnp.where(low, left, projected[1])
        values = jnp.where(low, right, left)
        gates = jnp.where(low, projected[1], right)
    position = lax.axis_index("tp")
    up_block = lax.dynamic_slice_in_dim(rank_up, position * key_cols, key_cols, 1)
    bias_block = lax.dynamic_slice_in_dim(decay_bias, position * key_cols, key_cols, 0)
    gain_block = lax.dynamic_slice_in_dim(head_gain, position * value_cols, value_cols, 0)
    mixed = pl.pallas_call(
        mixer_body,
        out_shape=jax.ShapeDtypeStruct((first.shape[0], value_cols), jnp.bfloat16),
        name="mixer",
    )(first, rank_rows, up_block, bias_block[None], qk, values, gates, gain_block[None])
    second = settle(
        columns_product([mixed], [output_shards]), tp_size, first, 1.0, gains[1], shifts[1]
    )
    last = settle(channel_mix(second), tp_size, second, 0.5, gains[2], shifts[2])
    return ring.restore(last, 1)


def solution(mesh):
    return jax.shard_map(
        functools.partial(per_device, dict(mesh.shape)),
        mesh=mesh,
        in_specs=(
            P(("rep", "fs"), None),
            P("fs", "tp"),
            P("fs", "tp"),
            P("tp", "fs"),
            P("fs", "tp"),
            P("fs", "tp"),
            P("fs", "tp"),
            P("fs", "tp"),
            P("tp", "fs"),
            P(),
            P(),
            P(),
            P(),
            P(),
            P(),
        ),
        out_specs=P(("rep", "fs"), None),
        check_vma=False,
    )
```
